32 devices in a mesh: grp: 2 (over x), ep: 16 (over z, y, core).
Axes of the slice: x: 2, y: 2, z: 4, core: 2. Of those that a mesh axis runs over, the one named last changes fastest.
Arguments:
- tokens: bfloat16 [512, 2048], P(('grp', 'ep')), parts along dimension 0, may hold values from -6 to 6
- norm_gain: bfloat16 [2048], replicated, may hold values from 0.099609375 to 1.8984375
- query_weight: bfloat16 [2048, 1024], P(None, 'ep'), may hold values from -0.125 to 0.125
- key_weight: bfloat16 [2048, 256], replicated, may hold values from -0.25 to 0.25
- value_weight: bfloat16 [2048, 256], replicated, may hold values from -0.125 to 0.125
- out_weight: bfloat16 [1024, 2048], P(None, 'ep'), may hold values from -0.1875 to 0.1875
- head_gain: bfloat16 [128], replicated, may hold values from 0.099609375 to 1.8984375
- lambdas: float32 [8], replicated, may hold values from 0.3 to 0.8
- cache_keys: bfloat16 [512, 1024, 2, 128], P(('grp', 'ep')), parts along dimension 0, may hold values from -1000 to 1000
- cache_values: bfloat16 [512, 1024, 2, 128], P(('grp', 'ep')), parts along dimension 0, may hold values from -6 to 6
- lengths: int32 [512], P(('grp', 'ep')), parts along dimension 0, may hold values from 64 to 1024
- moe_gain: bfloat16 [2048], replicated, may hold values from 0.099609375 to 1.8984375
- gate_weight: bfloat16 [16, 2048, 1024], P('ep'), may hold values from -0.375 to 0.375
- up_weight: bfloat16 [16, 2048, 1024], P('ep'), may hold values from -0.375 to 0.375
- down_weight: bfloat16 [16, 1024, 2048], P('ep'), may hold values from -0.02734375 to 0.02734375
- routes: int32 [512, 4], P(('grp', 'ep')), parts along dimension 0, may hold values from 0 to 15, all different within a row; in each aligned block of 16 rows (0 to 15, 16 to 31, ...) at most 8 rows name the same one
- route_weights: float32 [512, 4], P(('grp', 'ep')), parts along dimension 0, may hold values from 0.2 to 1
Outputs:
- mixed: bfloat16 [512, 2048], P(('grp', 'ep')), parts along dimension 0
The draws below stay inside these ranges and needn't reach their ends.
There are 2 independent parts, one for each index of `grp`. The reference program is written for one: setup_inputs(seed, part) draws one part's arguments, and reference() takes and returns one part's arrays. A program takes and returns all parts, laid end to end along the dimension named above; an argument that names none is the same for every part. Nothing has to cross between parts.
Inputs may be any that keep to these rules, and one draw needn't show every extreme that they name: `routes`: a token's 4 experts differ; the tokens of one device name each expert at most 8 times, and in every draw some expert is named exactly 8 times by one device's tokens.
All inputs are finite; a program needn't handle non-finite values.
Results may differ from the reference program's by a relative error of at most 0.034.
Values may be sent and summed in bfloat16 or wider, within the bound.
A program may use at most 128 MiB of HBM per device.

```python
import math
import jax
import jax.numpy as jnp
import numpy as np
from jax import lax

D = 2048
HEADS = 8
KV_HEADS = 2
DH = 64
VAL = 128
FF = 1024
TOPK = 4
SEQ_DEV = 16
CTX = 1024
EXPERTS = 16
CAP = 8
SEQS = 256
N_EP = 16


def draw_cache_keys(key, part):
    shape = (SEQS, CTX, KV_HEADS, 2 * DH)
    base = jax.random.normal(key, shape, jnp.float32) * 1.75
    return base.astype(jnp.bfloat16)


def plant(entries, stream_key, smallest, largest):
    longest = entries.shape.index(max(entries.shape))
    spots = []
    for shift in (0, 1):
        where = [jax.random.randint(jax.random.fold_in(stream_key, axis), (), 0, length) for axis, length in enumerate(entries.shape)]
        where[longest] = (where[longest] + shift) % entries.shape[longest]
        spots.append(tuple(where))
    return entries.at[spots[0]].set(smallest).at[spots[1]].set(largest)


def shard_levels(key, extent, cuts, low, top_value):
    def one(dim, parts):
        heights = jax.random.uniform(jax.random.fold_in(jax.random.fold_in(key, 6), dim), (parts,), jnp.float32, low / len(cuts), top_value / len(cuts))
        return jnp.repeat(jnp.exp(heights), extent[dim] // parts).reshape((-1,) + (1,) * (len(extent) - dim - 1))

    level = one(*cuts[0])
    for cut in cuts[1:]:
        level = level * one(*cut)
    return level


def shared_out(rng, own, number, rows, amount, top, reach, skew):
    ranking = jax.random.permutation(rng, amount)
    packed, common = portions_of(amount, rows * top, reach, skew, True), portions_of(amount, rows * top, reach, skew, False)
    places = jnp.arange(amount)

    def named(tallies, offset_by):
        used = int((tallies > 0).sum())
        fixed = max(1, used // 4)
        moved = fixed + (places - fixed + offset_by * (used - fixed)) % max(1, amount - fixed)
        return jnp.zeros((amount,), jnp.int32).at[ranking[jnp.where(places < fixed, places, moved)]].set(jnp.asarray(tallies, jnp.int32))

    tallies = jnp.where(number % 4 == 0, named(packed, number // 4), named(common, number - number // 4 - 1))
    mixed = jax.random.permutation(jax.random.fold_in(own, 3), amount)
    donor, taker = mixed[0:amount // 2 * 2:2], mixed[1:amount // 2 * 2:2]
    room = jnp.minimum(tallies[donor] - 1, reach - tallies[taker]) // 2
    room = jnp.where((donor == ranking[0]) | (taker == ranking[0]) | (tallies[taker] == 0), 0, jnp.maximum(room, 0))
    moved = jax.random.randint(jax.random.fold_in(own, 4), (amount // 2,), 0, 1 << 20) % (room + 1)
    tallies = tallies.at[donor].add(-moved).at[taker].add(moved)
    members = jnp.searchsorted(jnp.cumsum(tallies), jnp.arange(rows * top), side="right").astype(jnp.int32)
    listing = members.reshape(top, rows).T
    listing = listing[jax.random.permutation(jax.random.fold_in(own, 1), rows)]
    offset_by = jax.random.randint(jax.random.fold_in(own, 2), (rows, 1), 0, top)
    return jnp.take_along_axis(listing, (jnp.arange(top)[None, :] + offset_by) % top, axis=1)


def portions_of(amount, total, bound, lean, full):
    portions = [(1 << 20) // math.isqrt(standing ** lean) + 1 for standing in range(1, amount + 1)]
    largest = bound if full else min(bound, max(-(-total // amount), total * portions[0] // sum(portions)))
    least = 1 if total - largest >= amount - 1 else 0
    counts, surplus = [largest] + [least] * (amount - 1), total - largest - least * (amount - 1)
    while surplus > 0:
        candidates = [i for i in range(1, amount) if counts[i] < largest] or [i for i in range(1, amount) if counts[i] < bound]
        whole, budget = sum([portions[i] for i in candidates]), surplus
        for i in candidates:
            more = min(bound - counts[i], max(1, budget * portions[i] // whole), surplus)
            counts[i] = counts[i] + more
            surplus = surplus - more
    return np.array(counts)


def centred(rng, shape, scale, most, cuts=(), held_as=jnp.bfloat16):
    drawn = scale * jax.random.normal(rng, shape, jnp.float32)
    if cuts:
        drawn = drawn * shard_levels(rng, shape, cuts, -0.22, 0.18)
    return jnp.clip(drawn, -most, most).astype(held_as)


def setup_inputs(seed: int = 0, part: int = 0) -> dict:
    arg_keys = jax.random.split(jax.random.key(seed), 18)
    part_keys = jax.random.split(jax.random.fold_in(arg_keys[17], part), 18)
    tokens = centred(part_keys[0], (SEQS, D), 1.0, 6.0, ((0, 16),))
    norm_gain = jnp.clip(1.0 + 0.18 * jax.random.normal(arg_keys[1], (D,), jnp.float32), 0.099609375, 1.8984375).astype(jnp.bfloat16)
    query_weight = centred(arg_keys[2], (D, 2 * HEADS * DH), D ** -0.5, 0.125, ((1, 16),))
    key_weight = centred(arg_keys[3], (D, 2 * KV_HEADS * DH), (D // 4) ** -0.5, 0.25)
    value_weight = centred(arg_keys[4], (D, KV_HEADS * VAL), D ** -0.5, 0.125)
    out_weight = centred(arg_keys[5], (HEADS * VAL, D), (HEADS * VAL) ** -0.5, 0.1875, ((1, 16),))
    head_gain = jnp.clip(1.0 + 0.18 * jax.random.normal(arg_keys[6], (VAL,), jnp.float32), 0.099609375, 1.8984375).astype(jnp.bfloat16)
    lambdas = jnp.clip(jax.random.uniform(arg_keys[7], (HEADS,), jnp.float32, 0.3, 0.8), 0.3, 0.8)
    cache_keys = draw_cache_keys(jax.random.fold_in(jax.random.fold_in(arg_keys[17], part), 71), part)
    cache_values = centred(part_keys[9], (SEQS, CTX, KV_HEADS, VAL), 1.0, 6.0, ((0, 16),))
    lengths = plant(jax.random.randint(part_keys[10], (SEQS,), CTX // 16, CTX + 1), jax.random.fold_in(part_keys[10], 1), CTX // 16, CTX).astype(jnp.int32)
    moe_gain = jnp.clip(1.0 + 0.18 * jax.random.normal(arg_keys[11], (D,), jnp.float32), 0.099609375, 1.8984375).astype(jnp.bfloat16)
    gate_weight = centred(arg_keys[12], (EXPERTS, D, FF), (D // 9) ** -0.5, 0.375, ((0, 16),))
    up_weight = centred(arg_keys[13], (EXPERTS, D, FF), (D // 9) ** -0.5, 0.375, ((0, 16),))
    down_weight = centred(arg_keys[14], (EXPERTS, FF, D), (FF * 48) ** -0.5, 0.02734375, ((0, 16),))
    routes_keys = jax.random.split(jax.random.fold_in(part_keys[15], 1), SEQS // SEQ_DEV)
    routes_turns = jax.random.permutation(jax.random.fold_in(part_keys[15], 3), SEQS // SEQ_DEV)
    routes = jax.vmap(lambda own, number: shared_out(jax.random.fold_in(part_keys[15], 2), own, number, SEQ_DEV, EXPERTS, TOPK, CAP, 2))(routes_keys, routes_turns).reshape((SEQS, TOPK))
    route_weights = jnp.clip(0.2 + 0.8 * jax.random.uniform(part_keys[16], (SEQS, TOPK), jnp.float32) ** shard_levels(part_keys[16], (SEQS, TOPK), ((0, 16),), -0.2, 0.2), 0.2, 1.0)
    return dict(tokens=tokens, norm_gain=norm_gain, query_weight=query_weight, key_weight=key_weight, value_weight=value_weight, out_weight=out_weight, head_gain=head_gain, lambdas=lambdas, cache_keys=cache_keys, cache_values=cache_values, lengths=lengths, moe_gain=moe_gain, gate_weight=gate_weight, up_weight=up_weight, down_weight=down_weight, routes=routes, route_weights=route_weights)


epsilon = 1e-06
masked_score = -1e+30
clamp_limit = 7.0
swish_alpha = 1.702

def rms_scaled(values, gain):
    floats = values.astype(jnp.float32)
    return floats * lax.rsqrt(lax.optimization_barrier(jnp.mean(floats * floats, axis=-1, keepdims=True)) + epsilon) * gain.astype(jnp.float32)

def attention(queries, new_keys, new_values, cache_keys, cache_values, lengths, lambdas, head_gain):
    count = queries.shape[0]
    ctx_len = cache_keys.shape[1]
    kv_count = cache_keys.shape[2]
    head_dim = cache_keys.shape[3] // 2
    heads = lambdas.shape[0]
    group = heads // kv_count
    val_dim = cache_values.shape[3]
    query_grid = queries.reshape(count, kv_count, group, 2, head_dim).astype(jnp.float32)
    key_grid = cache_keys.reshape(count, ctx_len, kv_count, 2, head_dim).astype(jnp.float32)
    own_keys = new_keys.reshape(count, kv_count, 2, head_dim).astype(jnp.float32)
    inv_scale = head_dim ** (-0.5)
    scores = jnp.einsum('bkgcd,bjkcd->bkgcj', query_grid, key_grid) * inv_scale
    own_score = jnp.einsum('bkgcd,bkcd->bkgc', query_grid, own_keys) * inv_scale
    visible = jnp.arange(ctx_len, dtype=jnp.int32)[None, :] < lengths[:, None]
    scores = jnp.where(visible[:, None, None, None, :], scores, masked_score)
    highest = jnp.maximum(lax.optimization_barrier(jnp.max(scores, axis=-1)), own_score)
    expd = jnp.exp(scores - highest[..., None])
    own_exp = jnp.exp(own_score - highest)
    denominator = lax.optimization_barrier(jnp.sum(expd, axis=-1)) + own_exp
    probs = expd / denominator[..., None]
    own_prob = own_exp / denominator
    lambda_grid = lambdas.reshape(kv_count, group)[None, :, :]
    weights = (probs[:, :, :, 0] - lambda_grid[..., None] * probs[:, :, :, 1]).astype(jnp.bfloat16)
    own_weight = (own_prob[..., 0] - lambda_grid * own_prob[..., 1]).astype(jnp.bfloat16)
    attended = jnp.einsum('bkgj,bjkv->bkgv', weights.astype(jnp.float32), cache_values.astype(jnp.float32))
    own_vals = new_values.reshape(count, kv_count, val_dim).astype(jnp.float32)
    attended = attended + own_weight.astype(jnp.float32)[..., None] * own_vals[:, :, None, :]
    return rms_scaled(attended, head_gain).reshape(count, heads * val_dim).astype(jnp.bfloat16)

def expert_mlp(inputs, gate_w, up_w, down_w):
    gate = jnp.dot(inputs, gate_w, preferred_element_type=jnp.float32)
    upper = jnp.dot(inputs, up_w, preferred_element_type=jnp.float32)
    gate = jnp.minimum(gate, clamp_limit)
    upper = jnp.clip(upper, -clamp_limit, clamp_limit)
    act = ((upper + 1.0) * gate * jax.nn.sigmoid(swish_alpha * gate)).astype(jnp.bfloat16)
    return jnp.dot(act, down_w, preferred_element_type=jnp.float32).astype(jnp.bfloat16)

def reference(tokens, norm_gain, query_weight, key_weight, value_weight, out_weight, head_gain, lambdas, cache_keys, cache_values, lengths, moe_gain, gate_weight, up_weight, down_weight, routes, route_weights):
    count = tokens.shape[0]
    width = tokens.shape[1]
    normed = rms_scaled(tokens, norm_gain).astype(jnp.bfloat16)
    queries = jnp.dot(normed, query_weight, preferred_element_type=jnp.float32).astype(jnp.bfloat16)
    new_keys = jnp.dot(normed, key_weight, preferred_element_type=jnp.float32).astype(jnp.bfloat16)
    new_values = jnp.dot(normed, value_weight, preferred_element_type=jnp.float32).astype(jnp.bfloat16)
    head_out = attention(queries, new_keys, new_values, cache_keys, cache_values, lengths, lambdas, head_gain)
    attn_out = jnp.dot(head_out, out_weight, preferred_element_type=jnp.float32).astype(jnp.bfloat16)
    residual = (tokens.astype(jnp.float32) + attn_out.astype(jnp.float32)).astype(jnp.bfloat16)
    moe_in = rms_scaled(residual, moe_gain).astype(jnp.bfloat16)
    onehot = (routes.reshape(N_EP, SEQ_DEV * TOPK)[:, :, None] == jnp.arange(EXPERTS, dtype=jnp.int32)[None, None, :]).astype(jnp.int32)
    earlier = jnp.cumsum(onehot, axis=1) - onehot
    ranks = lax.optimization_barrier(jnp.sum(earlier * onehot, axis=2)).reshape(count, TOPK)
    block_of = jnp.broadcast_to((jnp.arange(count, dtype=jnp.int32) // SEQ_DEV)[:, None], (count, TOPK))
    slot_index = (routes * (N_EP * CAP) + block_of * CAP + ranks).astype(jnp.int32).reshape(-1)
    copies = jnp.broadcast_to(moe_in[:, None, :], (count, TOPK, width)).reshape(-1, width)
    buffer = jnp.zeros((EXPERTS * N_EP * CAP, width), jnp.bfloat16).at[slot_index].set(copies)
    buffer = buffer.reshape(EXPERTS, N_EP * CAP, width)
    results = lax.map(lambda group: expert_mlp(group[0], group[1], group[2], group[3]), (buffer, gate_weight, up_weight, down_weight))
    picked = results.reshape(-1, width)[slot_index].reshape(count, TOPK, width)
    moe_sum = lax.optimization_barrier(jnp.sum(route_weights[:, :, None] * picked.astype(jnp.float32), axis=1))
    return (residual.astype(jnp.float32) + moe_sum).astype(jnp.bfloat16)
```

```python
import functools

import jax
import jax.numpy as jnp
from jax import lax
from jax.experimental import pallas as pl
from jax.experimental.pallas import tpu as pltpu
from jax.sharding import PartitionSpec as P

epsilon = 1e-06
masked_score = -1e30
clamp_limit = 7.0
swish_alpha = 1.702
f32 = jnp.float32
bf16 = jnp.bfloat16


def rms_scaled(values, gain):
    floats = values.astype(f32)
    scale = lax.rsqrt(jnp.mean(floats * floats, axis=-1, keepdims=True) + epsilon)
    return floats * scale * gain.astype(f32)


def layer_kernel(
    n,
    tokens_ref,
    norm_gain_ref,
    head_gain_ref,
    moe_gain_ref,
    lambdas_ref,
    lengths_ref,
    shares_ref,
    wq_hbm,
    wk_hbm,
    wv_hbm,
    wo_hbm,
    keys_hbm,
    values_hbm,
    gate_hbm,
    up_hbm,
    down_hbm,
    out_ref,
    wq,
    wk,
    wv,
    wo,
    keys,
    values,
    gate_w,
    up_w,
    down_w,
    normed_all,
    heads_all,
    moe_all,
    q_out,
    q_in,
    ao_out,
    ao_in,
    shares_in,
    q_grid,
    own_k,
    own_v,
    ho_grid,
    residual,
    act,
    y_out,
    rs_sib,
    rs_y_send,
    rs_y,
    rs_z_send,
    rs_z,
    w_sem,
    k_sem,
    v_sem,
    send_sem,
    recv_sem,
):
    me = lax.axis_index("ep")
    A = n // 4
    a, b, c = me // 4, (me // 2) % 2, me % 2
    count, width = tokens_ref.shape
    heads = lambdas_ref.shape[0]
    ctx2, lanes = keys.shape[1], keys.shape[2]
    kv_count = wk.shape[1] // lanes
    group = heads // kv_count
    dh = lanes // 2
    val = values.shape[2]

    def idx(i, j, k):
        return (i * 2 + j) * 2 + k

    def fwd(d):
        return lax.rem(a + d, A)

    def back(d):
        return lax.rem(a - d + A, A)

    ydev, sdev = idx(a, 1 - b, c), idx(a, b, 1 - c)
    sent = []

    def remote(src, dst, k, j, dev):
        return pltpu.make_async_remote_copy(
            src_ref=src,
            dst_ref=dst,
            send_sem=send_sem.at[k, j],
            recv_sem=recv_sem.at[k, j],
            device_id={"ep": dev},
            device_id_type=pl.DeviceIdType.MESH,
        )

    def start(copy):
        copy.start()
        sent.append(copy)

    loads = [
        pltpu.make_async_copy(src, dst, w_sem.at[i])
        for i, (src, dst) in enumerate(
            [
                (wq_hbm, wq),
                (wk_hbm, wk),
                (wv_hbm, wv),
                (wo_hbm, wo),
                (gate_hbm.at[0], gate_w),
                (up_hbm.at[0], up_w),
                (down_hbm.at[0], down_w),
            ]
        )
    ]

    def key_load(s):
        return pltpu.make_async_copy(keys_hbm.at[s], keys.at[s], k_sem.at[s])

    def value_load(s):
        return pltpu.make_async_copy(values_hbm.at[s], values.at[s], v_sem.at[s])

    barrier = pltpu.get_barrier_semaphore()

    def greet(d, carry):
        pl.semaphore_signal(
            barrier,
            inc=1,
            device_id={"ep": lax.rem(me + d, n)},
            device_id_type=pl.DeviceIdType.MESH,
        )
        return carry

    lax.fori_loop(1, n, greet, 0)
    for i in range(4):
        loads[i].start()

    def cache_load(s, carry):
        key_load(s).start()
        value_load(s).start()
        return carry

    lax.fori_loop(0, count, cache_load, 0)
    for i in range(4, 7):
        loads[i].start()

    normed_all[me] = rms_scaled(tokens_ref[...], norm_gain_ref[...]).astype(bf16)
    pl.semaphore_wait(barrier, n - 1)

    def gather(buf, k):
        def cp(slot, j, dev):
            return remote(buf.at[slot], buf.at[slot], k, j, dev)

        for d in range(1, A):
            start(cp(me, d - 1, idx(fwd(d), b, c)))
        start(cp(me, A - 1, ydev))
        start(cp(me, 2 * A - 1, sdev))
        for d in range(1, A):
            slot = idx(back(d), b, c)
            cp(slot, d - 1, me).wait_recv()
            start(cp(slot, A - 1 + d, ydev))
            start(cp(slot, 2 * A - 1 + d, sdev))
        for d in range(A):
            slot = idx(back(d), 1 - b, c)
            cp(slot, A - 1 + d, me).wait_recv()
            start(cp(slot, 3 * A - 1 + d, sdev))
        for d in range(A):
            cp(idx(back(d), b, 1 - c), 2 * A - 1 + d, me).wait_recv()
        for d in range(A):
            cp(idx(back(d), 1 - b, 1 - c), 3 * A - 1 + d, me).wait_recv()

    def exchange_start(src, dst, k):
        def body(d, carry):
            peer = lax.rem(me + d, n)
            remote(src.at[peer], dst.at[me], k, d - 1, peer).start()
            return carry

        lax.fori_loop(1, n, body, 0)

    def exchange_wait(src, dst, k):
        def body(d, carry):
            peer = lax.rem(me - d + n, n)
            remote(src.at[peer], dst.at[peer], k, d - 1, peer).wait_recv()
            return carry

        lax.fori_loop(1, n, body, 0)

    def exchange_drain(src, dst, k):
        def body(d, carry):
            peer = lax.rem(me + d, n)
            remote(src.at[peer], dst.at[me], k, d - 1, peer).wait_send()
            return carry

        lax.fori_loop(1, n, body, 0)

    def spread(block):
        w = block.shape[1]
        if w == lanes:
            return block.astype(bf16)
        row = lax.broadcasted_iota(jnp.int32, (w, lanes), 0)
        col = lax.broadcasted_iota(jnp.int32, (w, lanes), 1)
        pick = (row + lax.rem(me * w, lanes) == col).astype(f32).astype(bf16)
        return jnp.dot(block.astype(bf16), pick, preferred_element_type=f32).astype(bf16)

    gather(normed_all, 0)
    exchange_start(shares_ref, shares_in, 6)
    shares_in[me] = shares_ref[me]
    loads[0].wait()
    q = jnp.dot(
        normed_all[...].reshape(n * count, width), wq[...], preferred_element_type=f32
    )
    q_out[...] = spread(q).reshape(n, count, lanes)
    exchange_start(q_out, q_in, 3)
    q_in[me] = q_out[me]
    loads[1].wait()
    loads[2].wait()
    mine = normed_all[me]
    own_k[:, 0, :] = jnp.dot(mine, wk[...], preferred_element_type=f32).astype(bf16).astype(f32)
    own_v[:, 0, :] = jnp.dot(mine, wv[...], preferred_element_type=f32).astype(bf16).astype(f32)
    exchange_wait(q_out, q_in, 3)
    parts = n // (2 * heads)
    for h in range(heads):
        for m in range(2):
            first = (2 * h + m) * parts
            total = q_in[first].astype(f32)
            for i in range(1, parts):
                total = total + q_in[first + i].astype(f32)
            q_grid[:, m * heads + h, :] = total

    inv_scale = dh ** (-0.5)
    rows = 2 * heads
    kv_of = lax.rem(lax.broadcasted_iota(jnp.int32, (rows, ctx2), 0), heads) // group
    column = lax.broadcasted_iota(jnp.int32, (rows, ctx2), 1)
    lam = lambdas_ref[...]
    row_kv = lax.rem(lax.broadcasted_iota(jnp.int32, (rows, lanes), 0), heads) // group
    head_gain = head_gain_ref[...].astype(f32)

    def attend(s, carry):
        key_load(s).wait()
        value_load(s).wait()
        qs = q_grid[s]
        own_key = jnp.zeros((rows, lanes), f32)
        own_val = jnp.zeros((heads, val), f32)
        for kv in range(kv_count):
            own_key = jnp.where(row_kv == kv, own_k[s, :, kv * lanes : (kv + 1) * lanes], own_key)
            own_val = jnp.where(
                row_kv[:heads] == kv, own_v[s, :, kv * val : (kv + 1) * val], own_val
            )
        own_score = jnp.sum(qs * own_key, axis=1, keepdims=True) * inv_scale
        scores = (
            lax.dot_general(
                qs.astype(bf16),
                keys[s],
                (((1,), (1,)), ((), ())),
                preferred_element_type=f32,
            )
            * inv_scale
        )
        limit = lengths_ref[s] * kv_count
        visible = (lax.rem(column, kv_count) == kv_of) & (column < limit)
        scores = jnp.where(visible, scores, masked_score)
        highest = jnp.maximum(jnp.max(scores, axis=1, keepdims=True), own_score)
        expd = jnp.exp(scores - highest)
        own_exp = jnp.exp(own_score - highest)
        inv = 1.0 / (jnp.sum(expd, axis=1, keepdims=True) + own_exp)
        probs = expd * inv
        own_prob = own_exp * inv
        weights = (probs[:heads] - lam * probs[heads:]).astype(bf16)
        own_weight = (own_prob[:heads] - lam * own_prob[heads:]).astype(bf16).astype(f32)
        attended = jnp.dot(weights, values[s], preferred_element_type=f32)
        attended = attended + own_weight * own_val
        ho_grid[s] = rms_scaled(attended, head_gain)
        return carry

    lax.fori_loop(0, count, attend, 0)
    for h in range(heads):
        heads_all[me, :, h * val : (h + 1) * val] = ho_grid[:, h, :].astype(bf16)

    gather(heads_all, 1)
    loads[3].wait()
    ao = jnp.dot(
        heads_all[...].reshape(n * count, heads * val), wo[...], preferred_element_type=f32
    )
    ao_out[...] = spread(ao).reshape(n, count, lanes)
    exchange_start(ao_out, ao_in, 4)
    ao_in[me] = ao_out[me]
    exchange_wait(ao_out, ao_in, 4)
    per = n * lanes // width
    for t in range(width // lanes):
        total = ao_in[t * per].astype(f32)
        for i in range(1, per):
            total = total + ao_in[t * per + i].astype(f32)
        cols = slice(t * lanes, (t + 1) * lanes)
        residual[:, cols] = (tokens_ref[:, cols].astype(f32) + total).astype(bf16).astype(f32)
    moe_all[me] = rms_scaled(residual[...], moe_gain_ref[...]).astype(bf16)

    gather(moe_all, 2)
    for i in range(4, 7):
        loads[i].wait()
    total_rows = n * count
    ff = gate_w.shape[1]
    tile = 256

    def hidden(i, carry):
        cols = pl.ds(pl.multiple_of(i * tile, tile), tile)
        x = moe_all[...].reshape(total_rows, width)
        gate = jnp.dot(x, gate_w[:, cols], preferred_element_type=f32)
        upper = jnp.dot(x, up_w[:, cols], preferred_element_type=f32)
        gate = jnp.minimum(gate, clamp_limit)
        upper = jnp.clip(upper, -clamp_limit, clamp_limit)
        act[:, cols] = ((upper + 1.0) * gate * jax.nn.sigmoid(swish_alpha * gate)).astype(bf16)
        return carry

    lax.fori_loop(0, ff // tile, hidden, 0)
    exchange_wait(shares_ref, shares_in, 6)
    diagonal = lax.broadcasted_iota(jnp.int32, (n, count, lanes), 1) == lax.broadcasted_iota(
        jnp.int32, (n, count, lanes), 2
    )
    share = jnp.sum(jnp.where(diagonal, shares_in[...], 0.0), axis=2, keepdims=True)
    share = share.reshape(total_rows, 1)

    def project(i, carry):
        cols = pl.ds(pl.multiple_of(i * tile, tile), tile)
        y = jnp.dot(act[...], down_w[:, cols], preferred_element_type=f32)
        y_out[:, :, cols] = (y * share).astype(bf16).reshape(n, count, tile)
        return carry

    lax.fori_loop(0, width // tile, project, 0)

    order = list(range(1, A)) + [0]

    def sib(d, j):
        return remote(
            y_out.at[idx(fwd(d), lax.rem(b + j, 2), 1 - c)],
            rs_sib.at[fwd(d) * 2 + lax.rem(b + j, 2)],
            5,
            2 * A - 1 + j * A + d,
            sdev,
        )

    for j in (1, 0):
        for d in order:
            start(sib(d, j))
    ycopies, zcopies = {}, {}
    for d in order:
        sib(d, 1).wait_recv()
        dest = fwd(d)
        rs_y_send[d] = (
            y_out[idx(dest, 1 - b, c)].astype(f32) + rs_sib[dest * 2 + 1 - b].astype(f32)
        ).astype(bf16)
        ycopies[d] = remote(rs_y_send.at[d], rs_y.at[d], 5, A - 1 + d, ydev)
        start(ycopies[d])
    total = residual[...]
    for d in order:
        sib(d, 0).wait_recv()
        ycopies[d].wait_recv()
        dest = fwd(d)
        part = (
            y_out[idx(dest, b, c)].astype(f32)
            + rs_sib[dest * 2 + b].astype(f32)
            + rs_y[d].astype(f32)
        )
        if d:
            rs_z_send[d - 1] = part.astype(bf16)
            zcopies[d] = remote(
                rs_z_send.at[d - 1], rs_z.at[d - 1], 5, d - 1, idx(dest, b, c)
            )
            start(zcopies[d])
        else:
            total = total + part
    for d in range(1, A):
        zcopies[d].wait_recv()
        total = total + rs_z[d - 1].astype(f32)
    out_ref[...] = total.astype(bf16)
    for copy in sent:
        copy.wait_send()
    exchange_drain(q_out, q_in, 3)
    exchange_drain(ao_out, ao_in, 4)
    exchange_drain(shares_ref, shares_in, 6)


def local(
    n,
    tokens,
    norm_gain,
    query_weight,
    key_weight,
    value_weight,
    out_weight,
    head_gain,
    lambdas,
    cache_keys,
    cache_values,
    lengths,
    moe_gain,
    gate_weight,
    up_weight,
    down_weight,
    routes,
    route_weights,
):
    count, width = tokens.shape
    heads = lambdas.shape[0]
    ctx, kv_count, lanes = cache_keys.shape[1:]
    val = cache_values.shape[3]
    ctx2 = ctx * kv_count
    ff = gate_weight.shape[2]
    A = n // 4
    experts = jnp.arange(n, dtype=jnp.int32)[:, None, None]
    shares = jnp.sum(jnp.where(routes[None] == experts, route_weights[None], 0.0), axis=2)
    shares = jnp.pad(shares, ((0, 0), (0, lanes - count)))[:, None, :]
    vmem = pl.BlockSpec(memory_space=pltpu.VMEM)
    smem = pl.BlockSpec(memory_space=pltpu.SMEM)
    hbm = pl.BlockSpec(memory_space=pl.ANY)
    scratch = [
        (query_weight.shape, bf16),
        (key_weight.shape, bf16),
        (value_weight.shape, bf16),
        (out_weight.shape, bf16),
        ((count, ctx2, lanes), bf16),
        ((count, ctx2, val), bf16),
        ((width, ff), bf16),
        ((width, ff), bf16),
        ((ff, width), bf16),
        ((n, count, width), bf16),
        ((n, count, heads * val), bf16),
        ((n, count, width), bf16),
        ((n, count, lanes), bf16),
        ((n, count, lanes), bf16),
        ((n, count, lanes), bf16),
        ((n, count, lanes), bf16),
        ((n, 1, lanes), f32),
        ((count, 2 * heads, lanes), f32),
        ((count, 1, kv_count * lanes), f32),
        ((count, 1, kv_count * val), f32),
        ((count, heads, val), f32),
        ((count, width), f32),
        ((n * count, ff), bf16),
        ((n, count, width), bf16),
        ((2 * A, count, width), bf16),
        ((A, count, width), bf16),
        ((A, count, width), bf16),
        ((A - 1, count, width), bf16),
        ((A - 1, count, width), bf16),
    ]
    return pl.pallas_call(
        functools.partial(layer_kernel, n),
        out_shape=jax.ShapeDtypeStruct((count, width), bf16),
        in_specs=[vmem] * 5 + [smem] + [vmem] + [hbm] * 9,
        out_specs=vmem,
        scratch_shapes=[pltpu.VMEM(s, t) for s, t in scratch]
        + [
            pltpu.SemaphoreType.DMA((7,)),
            pltpu.SemaphoreType.DMA((count,)),
            pltpu.SemaphoreType.DMA((count,)),
            pltpu.SemaphoreType.DMA((7, n - 1)),
            pltpu.SemaphoreType.DMA((7, n - 1)),
        ],
        compiler_params=pltpu.CompilerParams(
            collective_id=0, has_side_effects=True, vmem_limit_bytes=62 * 1024 * 1024
        ),
        name="layer",
    )(
        tokens,
        norm_gain.reshape(1, width),
        head_gain.reshape(1, val),
        moe_gain.reshape(1, width),
        lambdas.reshape(heads, 1),
        lengths,
        shares,
        query_weight,
        key_weight,
        value_weight,
        out_weight,
        cache_keys.reshape(count, ctx2, lanes),
        cache_values.reshape(count, ctx2, val),
        gate_weight,
        up_weight,
        down_weight,
    )


def solution(mesh):
    placed = (
        P(("grp", "ep"), None),
        P(),
        P(None, "ep"),
        P(),
        P(),
        P(None, "ep"),
        P(),
        P(),
        P(("grp", "ep"), None, None, None),
        P(("grp", "ep"), None, None, None),
        P(("grp", "ep")),
        P(),
        P("ep", None, None),
        P("ep", None, None),
        P("ep", None, None),
        P(("grp", "ep"), None),
        P(("grp", "ep"), None),
    )
    return jax.shard_map(
        functools.partial(local, mesh.shape["ep"]),
        mesh=mesh,
        in_specs=placed,
        out_specs=P(("grp", "ep"), None),
        check_vma=False,
    )
```

```python
import functools

import jax
import jax.numpy as jnp
from jax import lax
from jax.experimental import pallas as pl
from jax.experimental.pallas import tpu as pltpu
from jax.sharding import PartitionSpec as P

epsilon = 1e-06
masked_score = -1e30
clamp_limit = 7.0
swish_alpha = 1.702
f32 = jnp.float32
bf16 = jnp.bfloat16


def rms_scaled(values, gain):
    floats = values.astype(f32)
    scale = lax.rsqrt(jnp.mean(floats * floats, axis=-1, keepdims=True) + epsilon)
    return floats * scale * gain.astype(f32)


def layer_kernel(
    n,
    tokens_ref,
    norm_gain_ref,
    head_gain_ref,
    moe_gain_ref,
    lambdas_ref,
    lengths_ref,
    routes_ref,
    route_weights_ref,
    wq_hbm,
    wk_hbm,
    wv_hbm,
    wo_hbm,
    keys_hbm,
    values_hbm,
    gate_hbm,
    up_hbm,
    down_hbm,
    out_ref,
    wq,
    wk,
    wv,
    wo,
    keys,
    values,
    gate_w,
    up_w,
    down_w,
    normed_all,
    heads_all,
    moe_all,
    q_out,
    q_in,
    ao_out,
    ao_in,
    shares_out,
    shares_in,
    share,
    q_grid,
    own_k,
    own_v,
    ho_grid,
    residual,
    act,
    y_out,
    rs_sib,
    rs_y_send,
    rs_y,
    rs_z_send,
    rs_z,
    w_sem,
    k_sem,
    v_sem,
    send_sem,
    recv_sem,
):
    me = lax.axis_index("ep")
    A = n // 4
    a, b, c = me // 4, (me // 2) % 2, me % 2
    count, width = tokens_ref.shape
    heads = lambdas_ref.shape[0]
    ctx2, lanes = keys.shape[1], keys.shape[2]
    kv_count = wk.shape[1] // lanes
    group = heads // kv_count
    dh = lanes // 2
    val = values.shape[2]

    def idx(i, j, k):
        return (i * 2 + j) * 2 + k

    def fwd(d):
        return lax.rem(a + d, A)

    def back(d):
        return lax.rem(a - d + A, A)

    ydev, sdev = idx(a, 1 - b, c), idx(a, b, 1 - c)
    sent = []

    def remote(src, dst, k, j, dev):
        return pltpu.make_async_remote_copy(
            src_ref=src,
            dst_ref=dst,
            send_sem=send_sem.at[k, j],
            recv_sem=recv_sem.at[k, j],
            device_id={"ep": dev},
            device_id_type=pl.DeviceIdType.MESH,
        )

    def start(copy):
        copy.start()
        sent.append(copy)

    loads = [
        pltpu.make_async_copy(src, dst, w_sem.at[i])
        for i, (src, dst) in enumerate(
            [
                (wq_hbm, wq.at[b * 2 + c]),
                (wk_hbm, wk),
                (wv_hbm, wv),
                (wo_hbm, wo.at[b * 2 + c]),
                (gate_hbm.at[0], gate_w),
                (up_hbm.at[0], up_w),
                (down_hbm.at[0], down_w),
            ]
        )
    ]

    def key_load(s):
        return pltpu.make_async_copy(keys_hbm.at[s], keys.at[s], k_sem.at[s])

    def value_load(s):
        return pltpu.make_async_copy(values_hbm.at[s], values.at[s], v_sem.at[s])

    barrier = pltpu.get_barrier_semaphore()

    def greet(d, carry):
        pl.semaphore_signal(
            barrier,
            inc=1,
            device_id={"ep": lax.rem(me + d, n)},
            device_id_type=pl.DeviceIdType.MESH,
        )
        return carry

    lax.fori_loop(1, n, greet, 0)
    for i in (0, 3, 1, 2):
        loads[i].start()

    def cache_load(s, carry):
        key_load(s).start()
        value_load(s).start()
        return carry

    lax.fori_loop(0, count, cache_load, 0)
    for i in range(4, 7):
        loads[i].start()

    normed_all[a] = rms_scaled(
        tokens_ref[...], norm_gain_ref[...].reshape(1, width)
    ).astype(bf16)
    topk = routes_ref.shape[0]
    expert = lax.broadcasted_iota(jnp.int32, (n, count), 0)
    routed = jnp.zeros((n, count), f32)
    for k in range(topk):
        routed = routed + jnp.where(
            routes_ref[k : k + 1, :] == expert, route_weights_ref[k : k + 1, :], 0.0
        )
    shares_out[...] = jnp.zeros_like(shares_out)
    shares_out[:, 0, :count] = routed
    pl.semaphore_wait(barrier, n - 1)

    def share_weight(buf, k):
        own = b * 2 + c
        start(remote(buf.at[own], buf.at[own], k, 0, ydev))
        start(remote(buf.at[own], buf.at[own], k, 1, sdev))

    def share_weight_on(buf, k):
        other = (1 - b) * 2 + c
        remote(buf.at[other], buf.at[other], k, 0, ydev).wait_recv()
        start(remote(buf.at[other], buf.at[other], k, 2, sdev))

    def share_weight_wait(buf, k):
        for j in range(2):
            slot = lax.rem(b + j, 2) * 2 + 1 - c
            remote(buf.at[slot], buf.at[slot], k, 1 + j, sdev).wait_recv()

    def line_start(src, dst, k, same):
        for d in range(1, A):
            dev = idx(fwd(d), b, c)
            start(remote(src.at[a if same else fwd(d)], dst.at[a], k, d - 1, dev))

    def line_wait(dst, k):
        for d in range(1, A):
            slot = back(d)
            remote(dst.at[slot], dst.at[slot], k, d - 1, idx(slot, b, c)).wait_recv()

    def place(i, j, k):
        return (j * A + i) * 2 + k

    def exchange_start(src, dst, k):
        def body(d, carry):
            peer = lax.rem(me + d, n)
            remote(src.at[peer], dst.at[me], k, d - 1, peer).start()
            return carry

        lax.fori_loop(1, n, body, 0)

    def exchange_wait(src, dst, k):
        def body(d, carry):
            peer = lax.rem(me - d + n, n)
            remote(src.at[peer], dst.at[peer], k, d - 1, peer).wait_recv()
            return carry

        lax.fori_loop(1, n, body, 0)

    def exchange_drain(src, dst, k):
        def body(d, carry):
            peer = lax.rem(me + d, n)
            remote(src.at[peer], dst.at[me], k, d - 1, peer).wait_send()
            return carry

        lax.fori_loop(1, n, body, 0)

    line_start(normed_all, normed_all, 0, True)
    loads[0].wait()
    share_weight(wq, 7)
    loads[3].wait()
    share_weight(wo, 8)
    exchange_start(shares_out, shares_in, 6)
    shares_in[me] = shares_out[me]
    loads[1].wait()
    loads[2].wait()
    mine = normed_all[a]
    own_k[:, 0, :] = jnp.dot(mine, wk[...], preferred_element_type=f32).astype(bf16).astype(f32)
    own_v[:, 0, :] = jnp.dot(mine, wv[...], preferred_element_type=f32).astype(bf16).astype(f32)
    share_weight_on(wq, 7)
    line_wait(normed_all, 0)
    share_weight_wait(wq, 7)
    qw = wq.shape[1]
    q = lax.dot_general(
        normed_all[...].reshape(A * count, width),
        wq[...].reshape(4 * qw, width),
        (((1,), (1,)), ((), ())),
        preferred_element_type=f32,
    )
    q_out[...] = q.astype(bf16).reshape(A, count, 4 * qw)
    line_start(q_out, q_in, 3, False)
    q_in[a] = q_out[a]
    share_weight_on(wo, 8)
    line_wait(q_in, 3)
    per_block = 4 * qw // lanes
    lane_map = lax.broadcasted_iota(jnp.int32, (count, lanes), 1) // dh
    for h in range(heads):
        first = (h % per_block) * lanes
        both = q_in[h // per_block, :, first : first + lanes].astype(f32)
        for m in range(2):
            q_grid[:, m * heads + h, :] = jnp.where(lane_map == m, both, 0.0)

    inv_scale = dh ** (-0.5)
    rows = 2 * heads
    kv_of = lax.rem(lax.broadcasted_iota(jnp.int32, (rows, ctx2), 0), heads) // group
    column = lax.broadcasted_iota(jnp.int32, (rows, ctx2), 1)
    head_row = lax.broadcasted_iota(jnp.int32, (heads, 1), 0)
    lam = jnp.zeros((heads, 1), f32)
    for h in range(heads):
        lam = jnp.where(head_row == h, lambdas_ref[h], lam)
    matched = lax.rem(column, kv_count) == kv_of
    row_kv = lax.rem(lax.broadcasted_iota(jnp.int32, (rows, lanes), 0), heads) // group
    head_gain = head_gain_ref[...].astype(f32)
    step = 4 if count % 4 == 0 else 1

    def attend(i, carry):
        seqs = [i * step + u for u in range(step)]
        for s in seqs:
            key_load(s).wait()
            value_load(s).wait()
        queries = [q_grid[s] for s in seqs]
        scores = [
            lax.dot_general(
                qs.astype(bf16),
                keys[s],
                (((1,), (1,)), ((), ())),
                preferred_element_type=f32,
            )
            * inv_scale
            for s, qs in zip(seqs, queries)
        ]
        weights, own_parts = [], []
        for s, qs, score in zip(seqs, queries, scores):
            own_key = jnp.zeros((rows, lanes), f32)
            own_val = jnp.zeros((heads, val), f32)
            for kv in range(kv_count):
                own_key = jnp.where(
                    row_kv == kv, own_k[s, :, kv * lanes : (kv + 1) * lanes], own_key
                )
                own_val = jnp.where(
                    row_kv[:heads] == kv, own_v[s, :, kv * val : (kv + 1) * val], own_val
                )
            own_score = jnp.sum(qs * own_key, axis=1, keepdims=True) * inv_scale
            visible = matched & (column < lengths_ref[s] * kv_count)
            score = jnp.where(visible, score, masked_score)
            highest = jnp.maximum(jnp.max(score, axis=1, keepdims=True), own_score)
            expd = jnp.exp(score - highest)
            own_exp = jnp.exp(own_score - highest)
            inv = 1.0 / (jnp.sum(expd, axis=1, keepdims=True) + own_exp)
            own_prob = own_exp * inv
            weights.append(
                (expd[:heads] * inv[:heads] - expd[heads:] * (lam * inv[heads:])).astype(bf16)
            )
            own_weight = (own_prob[:heads] - lam * own_prob[heads:]).astype(bf16).astype(f32)
            own_parts.append(own_weight * own_val)
        sums = [
            jnp.dot(w, values[s], preferred_element_type=f32) for s, w in zip(seqs, weights)
        ]
        for s, attended, own in zip(seqs, sums, own_parts):
            ho_grid[s] = rms_scaled(attended + own, head_gain)
        return carry

    lax.fori_loop(0, count // step, attend, 0)
    for h in range(heads):
        heads_all[a, :, h * val : (h + 1) * val] = ho_grid[:, h, :].astype(bf16)

    line_start(heads_all, heads_all, 1, True)
    share_weight_wait(wo, 8)
    line_wait(heads_all, 1)
    ow = wo.shape[2]
    head_rows = heads_all[...].reshape(A * count, heads * val)
    ao = jnp.concatenate(
        [jnp.dot(head_rows, wo[j], preferred_element_type=f32) for j in range(4)], axis=1
    )
    ao_out[...] = ao.astype(bf16).reshape(A, count, 4 * ow)
    line_start(ao_out, ao_in, 4, False)
    ao_in[a] = ao_out[a]
    line_wait(ao_in, 4)
    for t in range(A):
        cols = slice(t * 4 * ow, (t + 1) * 4 * ow)
        residual[:, cols] = (
            (tokens_ref[:, cols].astype(f32) + ao_in[t].astype(f32)).astype(bf16).astype(f32)
        )

    mine_at = place(a, b, c)
    moe_all[mine_at] = rms_scaled(residual[...], moe_gain_ref[...].reshape(1, width)).astype(bf16)

    def cp(slot, j, dev):
        return remote(moe_all.at[slot], moe_all.at[slot], 2, j, dev)

    for d in range(1, A):
        start(cp(mine_at, d - 1, idx(fwd(d), b, c)))
    start(cp(mine_at, A - 1, ydev))
    start(cp(mine_at, 2 * A - 1, sdev))
    for d in range(1, A):
        slot = place(back(d), b, c)
        cp(slot, d - 1, me).wait_recv()
        start(cp(slot, A - 1 + d, ydev))
        start(cp(slot, 2 * A - 1 + d, sdev))
    for i in range(4, 7):
        loads[i].wait()
    for d in range(A):
        cp(place(back(d), b, 1 - c), 2 * A - 1 + d, me).wait_recv()
    half = 2 * A
    half_rows = half * count
    ff = gate_w.shape[1]
    tile = 256

    def hidden(which):
        def body(i, carry):
            cols = pl.ds(pl.multiple_of(i * tile, tile), tile)
            x = moe_all[pl.ds(which * half, half)].reshape(half_rows, width)
            gate = jnp.dot(x, gate_w[:, cols], preferred_element_type=f32)
            upper = jnp.dot(x, up_w[:, cols], preferred_element_type=f32)
            gate = jnp.minimum(gate, clamp_limit)
            upper = jnp.clip(upper, -clamp_limit, clamp_limit)
            value = (upper + 1.0) * gate * jax.nn.sigmoid(swish_alpha * gate)
            act[which, :, cols] = value.astype(bf16)
            return carry

        lax.fori_loop(0, ff // tile, body, 0)

    hidden(b)
    for d in range(A):
        slot = place(back(d), 1 - b, c)
        cp(slot, A - 1 + d, me).wait_recv()
        start(cp(slot, 3 * A - 1 + d, sdev))
    exchange_wait(shares_out, shares_in, 6)
    diagonal = lax.broadcasted_iota(jnp.int32, (count, lanes), 0) == lax.broadcasted_iota(
        jnp.int32, (count, lanes), 1
    )
    for i in range(A):
        for j in range(2):
            for k in range(2):
                row = shares_in[idx(i, j, k)]
                share[place(i, j, k)] = jnp.sum(
                    jnp.where(diagonal, row, 0.0), axis=1, keepdims=True
                )
    for d in range(A):
        cp(place(back(d), 1 - b, 1 - c), 3 * A - 1 + d, me).wait_recv()
    hidden(1 - b)

    def project(which):
        part = share[pl.ds(which * half, half)].reshape(half_rows, 1)

        def body(i, carry):
            cols = pl.ds(pl.multiple_of(i * tile, tile), tile)
            y = jnp.dot(act[which], down_w[:, cols], preferred_element_type=f32)
            y_out[pl.ds(which * half, half), :, cols] = (
                (y * part).astype(bf16).reshape(half, count, tile)
            )
            return carry

        lax.fori_loop(0, width // tile, body, 0)

    order = list(range(1, A)) + [0]

    def sib(d, j):
        return remote(
            y_out.at[place(fwd(d), lax.rem(b + j, 2), 1 - c)],
            rs_sib.at[fwd(d) * 2 + lax.rem(b + j, 2)],
            5,
            2 * A - 1 + j * A + d,
            sdev,
        )

    for j in (1, 0):
        project(lax.rem(b + j, 2))
        for d in order:
            start(sib(d, j))
    ycopies, zcopies = {}, {}
    for d in order:
        sib(d, 1).wait_recv()
        dest = fwd(d)
        rs_y_send[d] = (
            y_out[place(dest, 1 - b, c)].astype(f32) + rs_sib[dest * 2 + 1 - b].astype(f32)
        ).astype(bf16)
        ycopies[d] = remote(rs_y_send.at[d], rs_y.at[d], 5, A - 1 + d, ydev)
        start(ycopies[d])
    total = residual[...]
    for d in order:
        sib(d, 0).wait_recv()
        ycopies[d].wait_recv()
        dest = fwd(d)
        part = (
            y_out[place(dest, b, c)].astype(f32)
            + rs_sib[dest * 2 + b].astype(f32)
            + rs_y[d].astype(f32)
        )
        if d:
            rs_z_send[d - 1] = part.astype(bf16)
            zcopies[d] = remote(
                rs_z_send.at[d - 1], rs_z.at[d - 1], 5, d - 1, idx(dest, b, c)
            )
            start(zcopies[d])
        else:
            total = total + part
    for d in range(1, A):
        zcopies[d].wait_recv()
        total = total + rs_z[d - 1].astype(f32)
    out_ref[...] = total.astype(bf16)
    for copy in sent:
        copy.wait_send()
    exchange_drain(shares_out, shares_in, 6)


def local(
    n,
    tokens,
    norm_gain,
    query_weight,
    key_weight,
    value_weight,
    out_weight,
    head_gain,
    lambdas,
    cache_keys,
    cache_values,
    lengths,
    moe_gain,
    gate_weight,
    up_weight,
    down_weight,
    routes,
    route_weights,
):
    count, width = tokens.shape
    heads = lambdas.shape[0]
    ctx, kv_count, lanes = cache_keys.shape[1:]
    val = cache_values.shape[3]
    ctx2 = ctx * kv_count
    ff = gate_weight.shape[2]
    A = n // 4
    vmem = pl.BlockSpec(memory_space=pltpu.VMEM)
    smem = pl.BlockSpec(memory_space=pltpu.SMEM)
    hbm = pl.BlockSpec(memory_space=pl.ANY)
    scratch = [
        ((4,) + query_weight.shape[::-1], bf16),
        (key_weight.shape, bf16),
        (value_weight.shape, bf16),
        ((4,) + out_weight.shape, bf16),
        ((count, ctx2, lanes), bf16),
        ((count, ctx2, val), bf16),
        ((width, ff), bf16),
        ((width, ff), bf16),
        ((ff, width), bf16),
        ((A, count, width), bf16),
        ((A, count, heads * val), bf16),
        ((n, count, width), bf16),
        ((A, count, 4 * query_weight.shape[1]), bf16),
        ((A, count, 4 * query_weight.shape[1]), bf16),
        ((A, count, 4 * out_weight.shape[1]), bf16),
        ((A, count, 4 * out_weight.shape[1]), bf16),
        ((n, 1, lanes), f32),
        ((n, 1, lanes), f32),
        ((n, count, 1), f32),
        ((count, 2 * heads, lanes), f32),
        ((count, 1, kv_count * lanes), f32),
        ((count, 1, kv_count * val), f32),
        ((count, heads, val), f32),
        ((count, width), f32),
        ((2, n * count // 2, ff), bf16),
        ((n, count, width), bf16),
        ((2 * A, count, width), bf16),
        ((A, count, width), bf16),
        ((A, count, width), bf16),
        ((A - 1, count, width), bf16),
        ((A - 1, count, width), bf16),
    ]
    return pl.pallas_call(
        functools.partial(layer_kernel, n),
        out_shape=jax.ShapeDtypeStruct((count, width), bf16),
        in_specs=[vmem] * 4 + [smem] * 2 + [vmem] * 2 + [hbm] * 9,
        out_specs=vmem,
        scratch_shapes=[pltpu.VMEM(s, t) for s, t in scratch]
        + [
            pltpu.SemaphoreType.DMA((7,)),
            pltpu.SemaphoreType.DMA((count,)),
            pltpu.SemaphoreType.DMA((count,)),
            pltpu.SemaphoreType.DMA((9, n - 1)),
            pltpu.SemaphoreType.DMA((9, n - 1)),
        ],
        compiler_params=pltpu.CompilerParams(
            collective_id=0, has_side_effects=True, vmem_limit_bytes=62 * 1024 * 1024
        ),
        name="layer",
    )(
        tokens,
        norm_gain,
        head_gain.reshape(1, val),
        moe_gain,
        lambdas,
        lengths,
        routes.T,
        route_weights.T,
        query_weight.T,
        key_weight,
        value_weight,
        out_weight,
        cache_keys.reshape(count, ctx2, lanes),
        cache_values.reshape(count, ctx2, val),
        gate_weight,
        up_weight,
        down_weight,
    )


def solution(mesh):
    placed = (
        P(("grp", "ep"), None),
        P(),
        P(None, "ep"),
        P(),
        P(),
        P(None, "ep"),
        P(),
        P(),
        P(("grp", "ep"), None, None, None),
        P(("grp", "ep"), None, None, None),
        P(("grp", "ep")),
        P(),
        P("ep", None, None),
        P("ep", None, None),
        P("ep", None, None),
        P(("grp", "ep"), None),
        P(("grp", "ep"), None),
    )
    return jax.shard_map(
        functools.partial(local, mesh.shape["ep"]),
        mesh=mesh,
        in_specs=placed,
        out_specs=P(("grp", "ep"), None),
        check_vma=False,
    )
```

```python
import functools

import jax
import jax.numpy as jnp
from jax import lax
from jax.experimental import pallas as pl
from jax.experimental.pallas import tpu as pltpu
from jax.sharding import PartitionSpec as P

epsilon = 1e-06
masked_score = -1e30
clamp_limit = 7.0
swish_alpha = 1.702
f32 = jnp.float32
bf16 = jnp.bfloat16


def rms_scaled(values, gain):
    floats = values.astype(f32)
    scale = lax.rsqrt(jnp.mean(floats * floats, axis=-1, keepdims=True) + epsilon)
    return floats * scale * gain.astype(f32)


def layer_kernel(
    n,
    tokens_ref,
    norm_gain_ref,
    head_gain_ref,
    moe_gain_ref,
    lambdas_ref,
    lengths_ref,
    routes_ref,
    route_weights_ref,
    wq_hbm,
    wk_hbm,
    wv_hbm,
    wo_hbm,
    keys_hbm,
    values_hbm,
    gate_hbm,
    up_hbm,
    down_hbm,
    out_ref,
    wq,
    wk,
    wv,
    wo,
    keys,
    values,
    gate_w,
    up_w,
    down_w,
    normed_all,
    heads_all,
    moe_all,
    q_out,
    q_in,
    ao_out,
    ao_in,
    shares_out,
    shares_in,
    share,
    q_grid,
    own_k,
    own_v,
    ho_grid,
    residual,
    act,
    y_out,
    rs_sib,
    rs_y_send,
    rs_y,
    rs_z_send,
    rs_z,
    w_sem,
    k_sem,
    v_sem,
    send_sem,
    recv_sem,
):
    me = lax.axis_index("ep")
    A = n // 4
    a, b, c = me // 4, (me // 2) % 2, me % 2
    count, width = tokens_ref.shape
    heads = lambdas_ref.shape[0]
    ctx2, lanes = keys.shape[1], keys.shape[2]
    kv_count = wk.shape[1] // lanes
    group = heads // kv_count
    dh = lanes // 2
    val = values.shape[2]

    def idx(i, j, k):
        return (i * 2 + j) * 2 + k

    def fwd(d):
        return lax.rem(a + d, A)

    def back(d):
        return lax.rem(a - d + A, A)

    ydev, sdev = idx(a, 1 - b, c), idx(a, b, 1 - c)
    sent = []

    def remote(src, dst, k, j, dev):
        return pltpu.make_async_remote_copy(
            src_ref=src,
            dst_ref=dst,
            send_sem=send_sem.at[k, j],
            recv_sem=recv_sem.at[k, j],
            device_id={"ep": dev},
            device_id_type=pl.DeviceIdType.MESH,
        )

    def start(copy):
        copy.start()
        sent.append(copy)

    loads = [
        pltpu.make_async_copy(src, dst, w_sem.at[i])
        for i, (src, dst) in enumerate(
            [
                (wq_hbm, wq.at[b * 2 + c]),
                (wk_hbm, wk),
                (wv_hbm, wv),
                (wo_hbm, wo.at[b * 2 + c]),
                (gate_hbm.at[0], gate_w),
                (up_hbm.at[0], up_w),
                (down_hbm.at[0], down_w),
            ]
        )
    ]

    def key_load(s):
        return pltpu.make_async_copy(keys_hbm.at[s], keys.at[s], k_sem.at[s])

    def value_load(s):
        return pltpu.make_async_copy(values_hbm.at[s], values.at[s], v_sem.at[s])

    barrier = pltpu.get_barrier_semaphore()

    def greet(d, carry):
        pl.semaphore_signal(
            barrier,
            inc=1,
            device_id={"ep": lax.rem(me + d, n)},
            device_id_type=pl.DeviceIdType.MESH,
        )
        return carry

    lax.fori_loop(1, n, greet, 0)
    for i in (0, 3, 1, 2):
        loads[i].start()

    def cache_load(s, carry):
        key_load(s).start()
        value_load(s).start()
        return carry

    lax.fori_loop(0, count, cache_load, 0)
    for i in range(4, 7):
        loads[i].start()

    normed_all[a] = rms_scaled(
        tokens_ref[...], norm_gain_ref[...].reshape(1, width)
    ).astype(bf16)
    topk = routes_ref.shape[0]
    expert = lax.broadcasted_iota(jnp.int32, (n, count), 0)
    routed = jnp.zeros((n, count), f32)
    for k in range(topk):
        routed = routed + jnp.where(
            routes_ref[k : k + 1, :] == expert, route_weights_ref[k : k + 1, :], 0.0
        )
    shares_out[...] = jnp.zeros_like(shares_out)
    shares_out[:, 0, :count] = routed
    pl.semaphore_wait(barrier, n - 1)

    def share_weight(buf, k):
        own = b * 2 + c
        start(remote(buf.at[own], buf.at[own], k, 0, ydev))
        start(remote(buf.at[own], buf.at[own], k, 1, sdev))

    def share_weight_on(buf, k):
        other = (1 - b) * 2 + c
        remote(buf.at[other], buf.at[other], k, 0, ydev).wait_recv()
        start(remote(buf.at[other], buf.at[other], k, 2, sdev))

    def share_weight_wait(buf, k):
        for j in range(2):
            slot = lax.rem(b + j, 2) * 2 + 1 - c
            remote(buf.at[slot], buf.at[slot], k, 1 + j, sdev).wait_recv()

    def line_start(src, dst, k, same):
        for d in range(1, A):
            dev = idx(fwd(d), b, c)
            start(remote(src.at[a if same else fwd(d)], dst.at[a], k, d - 1, dev))

    def line_wait(dst, k):
        for d in range(1, A):
            slot = back(d)
            remote(dst.at[slot], dst.at[slot], k, d - 1, idx(slot, b, c)).wait_recv()

    def place(i, j, k):
        return (j * A + i) * 2 + k

    def exchange_start(src, dst, k):
        def body(d, carry):
            peer = lax.rem(me + d, n)
            remote(src.at[peer], dst.at[me], k, d - 1, peer).start()
            return carry

        lax.fori_loop(1, n, body, 0)

    def exchange_wait(src, dst, k):
        def body(d, carry):
            peer = lax.rem(me - d + n, n)
            remote(src.at[peer], dst.at[peer], k, d - 1, peer).wait_recv()
            return carry

        lax.fori_loop(1, n, body, 0)

    def exchange_drain(src, dst, k):
        def body(d, carry):
            peer = lax.rem(me + d, n)
            remote(src.at[peer], dst.at[me], k, d - 1, peer).wait_send()
            return carry

        lax.fori_loop(1, n, body, 0)

    line_start(normed_all, normed_all, 0, True)
    loads[0].wait()
    share_weight(wq, 7)
    loads[3].wait()
    share_weight(wo, 8)
    exchange_start(shares_out, shares_in, 6)
    shares_in[me] = shares_out[me]
    loads[1].wait()
    loads[2].wait()
    mine = normed_all[a]
    own_k[:, 0, :] = jnp.dot(mine, wk[...], preferred_element_type=f32).astype(bf16).astype(f32)
    own_v[:, 0, :] = jnp.dot(mine, wv[...], preferred_element_type=f32).astype(bf16).astype(f32)
    share_weight_on(wq, 7)
    line_wait(normed_all, 0)
    share_weight_wait(wq, 7)
    qw = wq.shape[1]
    q = lax.dot_general(
        normed_all[...].reshape(A * count, width),
        wq[...].reshape(4 * qw, width),
        (((1,), (1,)), ((), ())),
        preferred_element_type=f32,
    )
    q_out[...] = q.astype(bf16).reshape(A, count, 4 * qw)
    line_start(q_out, q_in, 3, False)
    q_in[a] = q_out[a]
    share_weight_on(wo, 8)
    line_wait(q_in, 3)
    per_block = 4 * qw // lanes
    lane_map = lax.broadcasted_iota(jnp.int32, (count, lanes), 1) // dh
    for h in range(heads):
        first = (h % per_block) * lanes
        both = q_in[h // per_block, :, first : first + lanes].astype(f32)
        for m in range(2):
            q_grid[:, m * heads + h, :] = jnp.where(lane_map == m, both, 0.0)

    inv_scale = dh ** (-0.5)
    rows = 2 * heads
    kv_of = lax.rem(lax.broadcasted_iota(jnp.int32, (rows, ctx2), 0), heads) // group
    column = lax.broadcasted_iota(jnp.int32, (rows, ctx2), 1)
    head_row = lax.broadcasted_iota(jnp.int32, (heads, 1), 0)
    lam = jnp.zeros((heads, 1), f32)
    for h in range(heads):
        lam = jnp.where(head_row == h, lambdas_ref[h], lam)
    matched = lax.rem(column, kv_count) == kv_of
    row_kv = lax.rem(lax.broadcasted_iota(jnp.int32, (rows, lanes), 0), heads) // group
    head_gain = head_gain_ref[...].astype(f32)
    step = 4 if count % 4 == 0 else 1

    def attend(i, carry):
        seqs = [i * step + u for u in range(step)]
        for s in seqs:
            key_load(s).wait()
            value_load(s).wait()
        queries = [q_grid[s] for s in seqs]
        scores = [
            lax.dot_general(
                qs.astype(bf16),
                keys[s],
                (((1,), (1,)), ((), ())),
                preferred_element_type=f32,
            )
            * inv_scale
            for s, qs in zip(seqs, queries)
        ]
        weights, own_parts = [], []
        for s, qs, score in zip(seqs, queries, scores):
            own_key = jnp.zeros((rows, lanes), f32)
            own_val = jnp.zeros((heads, val), f32)
            for kv in range(kv_count):
                own_key = jnp.where(
                    row_kv == kv, own_k[s, :, kv * lanes : (kv + 1) * lanes], own_key
                )
                own_val = jnp.where(
                    row_kv[:heads] == kv, own_v[s, :, kv * val : (kv + 1) * val], own_val
                )
            own_score = jnp.sum(qs * own_key, axis=1, keepdims=True) * inv_scale
            visible = matched & (column < lengths_ref[s] * kv_count)
            score = jnp.where(visible, score, masked_score)
            highest = jnp.maximum(jnp.max(score, axis=1, keepdims=True), own_score)
            expd = jnp.exp(score - highest)
            own_exp = jnp.exp(own_score - highest)
            inv = 1.0 / (jnp.sum(expd, axis=1, keepdims=True) + own_exp)
            own_prob = own_exp * inv
            weights.append(
                (expd[:heads] * inv[:heads] - expd[heads:] * (lam * inv[heads:])).astype(bf16)
            )
            own_weight = (own_prob[:heads] - lam * own_prob[heads:]).astype(bf16).astype(f32)
            own_parts.append(own_weight * own_val)
        sums = [
            jnp.dot(w, values[s], preferred_element_type=f32) for s, w in zip(seqs, weights)
        ]
        for s, attended, own in zip(seqs, sums, own_parts):
            ho_grid[s] = rms_scaled(attended + own, head_gain)
        return carry

    lax.fori_loop(0, count // step, attend, 0)
    for h in range(heads):
        heads_all[a, :, h * val : (h + 1) * val] = ho_grid[:, h, :].astype(bf16)

    line_start(heads_all, heads_all, 1, True)
    share_weight_wait(wo, 8)
    line_wait(heads_all, 1)
    ow = wo.shape[2]
    head_rows = heads_all[...].reshape(A * count, heads * val)
    ao = jnp.concatenate(
        [jnp.dot(head_rows, wo[j], preferred_element_type=f32) for j in range(4)], axis=1
    )
    ao_out[...] = ao.astype(bf16).reshape(A, count, 4 * ow)
    line_start(ao_out, ao_in, 4, False)
    ao_in[a] = ao_out[a]
    line_wait(ao_in, 4)
    for t in range(A):
        cols = slice(t * 4 * ow, (t + 1) * 4 * ow)
        residual[:, cols] = (
            (tokens_ref[:, cols].astype(f32) + ao_in[t].astype(f32)).astype(bf16).astype(f32)
        )

    mine_at = place(a, b, c)
    moe_all[mine_at] = rms_scaled(residual[...], moe_gain_ref[...].reshape(1, width)).astype(bf16)

    def cp(slot, j, dev):
        return remote(moe_all.at[slot], moe_all.at[slot], 2, j, dev)

    for d in range(1, A):
        start(cp(mine_at, d - 1, idx(fwd(d), b, c)))
    start(cp(mine_at, A - 1, ydev))
    start(cp(mine_at, 2 * A - 1, sdev))
    for d in range(1, A):
        slot = place(back(d), b, c)
        cp(slot, d - 1, me).wait_recv()
        start(cp(slot, A - 1 + d, ydev))
        start(cp(slot, 2 * A - 1 + d, sdev))
    for i in range(4, 7):
        loads[i].wait()
    for d in range(A):
        cp(place(back(d), b, 1 - c), 2 * A - 1 + d, me).wait_recv()
    half = 2 * A
    half_rows = half * count
    ff = gate_w.shape[1]
    tile = 256

    def hidden(which):
        def body(i, carry):
            cols = pl.ds(pl.multiple_of(i * tile, tile), tile)
            x = moe_all[pl.ds(which * half, half)].reshape(half_rows, width)
            gate = jnp.dot(x, gate_w[:, cols], preferred_element_type=f32)
            upper = jnp.dot(x, up_w[:, cols], preferred_element_type=f32)
            gate = jnp.minimum(gate, clamp_limit)
            upper = jnp.clip(upper, -clamp_limit, clamp_limit)
            value = (upper + 1.0) * gate * jax.nn.sigmoid(swish_alpha * gate)
            act[which, :, cols] = value.astype(bf16)
            return carry

        lax.fori_loop(0, ff // tile, body, 0)

    hidden(b)
    for d in range(A):
        slot = place(back(d), 1 - b, c)
        cp(slot, A - 1 + d, me).wait_recv()
        start(cp(slot, 3 * A - 1 + d, sdev))
    exchange_wait(shares_out, shares_in, 6)
    diagonal = lax.broadcasted_iota(jnp.int32, (count, lanes), 0) == lax.broadcasted_iota(
        jnp.int32, (count, lanes), 1
    )
    for i in range(A):
        for j in range(2):
            for k in range(2):
                row = shares_in[idx(i, j, k)]
                share[place(i, j, k)] = jnp.sum(
                    jnp.where(diagonal, row, 0.0), axis=1, keepdims=True
                )
    def project(which):
        part = share[pl.ds(which * half, half)].reshape(half_rows, 1)

        def body(i, carry):
            cols = pl.ds(pl.multiple_of(i * tile, tile), tile)
            y = jnp.dot(act[which], down_w[:, cols], preferred_element_type=f32)
            y_out[pl.ds(which * half, half), :, cols] = (
                (y * part).astype(bf16).reshape(half, count, tile)
            )
            return carry

        lax.fori_loop(0, width // tile, body, 0)

    order = list(range(1, A)) + [0]

    def sib(d, j):
        return remote(
            y_out.at[place(fwd(d), lax.rem(b + j, 2), 1 - c)],
            rs_sib.at[fwd(d) * 2 + lax.rem(b + j, 2)],
            5,
            2 * A - 1 + j * A + d,
            sdev,
        )

    project(b)
    for d in order:
        start(sib(d, 0))
    for d in range(A):
        cp(place(back(d), 1 - b, 1 - c), 3 * A - 1 + d, me).wait_recv()
    hidden(1 - b)
    project(1 - b)
    for d in order:
        start(sib(d, 1))
    ycopies, zcopies = {}, {}
    for d in order:
        sib(d, 1).wait_recv()
        dest = fwd(d)
        rs_y_send[d] = (
            y_out[place(dest, 1 - b, c)].astype(f32) + rs_sib[dest * 2 + 1 - b].astype(f32)
        ).astype(bf16)
        ycopies[d] = remote(rs_y_send.at[d], rs_y.at[d], 5, A - 1 + d, ydev)
        start(ycopies[d])
    total = residual[...]
    for d in order:
        sib(d, 0).wait_recv()
        ycopies[d].wait_recv()
        dest = fwd(d)
        part = (
            y_out[place(dest, b, c)].astype(f32)
            + rs_sib[dest * 2 + b].astype(f32)
            + rs_y[d].astype(f32)
        )
        if d:
            rs_z_send[d - 1] = part.astype(bf16)
            zcopies[d] = remote(
                rs_z_send.at[d - 1], rs_z.at[d - 1], 5, d - 1, idx(dest, b, c)
            )
            start(zcopies[d])
        else:
            total = total + part
    for d in range(1, A):
        zcopies[d].wait_recv()
        total = total + rs_z[d - 1].astype(f32)
    out_ref[...] = total.astype(bf16)
    for copy in sent:
        copy.wait_send()
    exchange_drain(shares_out, shares_in, 6)


def local(
    n,
    tokens,
    norm_gain,
    query_weight,
    key_weight,
    value_weight,
    out_weight,
    head_gain,
    lambdas,
    cache_keys,
    cache_values,
    lengths,
    moe_gain,
    gate_weight,
    up_weight,
    down_weight,
    routes,
    route_weights,
):
    count, width = tokens.shape
    heads = lambdas.shape[0]
    ctx, kv_count, lanes = cache_keys.shape[1:]
    val = cache_values.shape[3]
    ctx2 = ctx * kv_count
    ff = gate_weight.shape[2]
    A = n // 4
    vmem = pl.BlockSpec(memory_space=pltpu.VMEM)
    smem = pl.BlockSpec(memory_space=pltpu.SMEM)
    hbm = pl.BlockSpec(memory_space=pl.ANY)
    scratch = [
        ((4,) + query_weight.shape[::-1], bf16),
        (key_weight.shape, bf16),
        (value_weight.shape, bf16),
        ((4,) + out_weight.shape, bf16),
        ((count, ctx2, lanes), bf16),
        ((count, ctx2, val), bf16),
        ((width, ff), bf16),
        ((width, ff), bf16),
        ((ff, width), bf16),
        ((A, count, width), bf16),
        ((A, count, heads * val), bf16),
        ((n, count, width), bf16),
        ((A, count, 4 * query_weight.shape[1]), bf16),
        ((A, count, 4 * query_weight.shape[1]), bf16),
        ((A, count, 4 * out_weight.shape[1]), bf16),
        ((A, count, 4 * out_weight.shape[1]), bf16),
        ((n, 1, lanes), f32),
        ((n, 1, lanes), f32),
        ((n, count, 1), f32),
        ((count, 2 * heads, lanes), f32),
        ((count, 1, kv_count * lanes), f32),
        ((count, 1, kv_count * val), f32),
        ((count, heads, val), f32),
        ((count, width), f32),
        ((2, n * count // 2, ff), bf16),
        ((n, count, width), bf16),
        ((2 * A, count, width), bf16),
        ((A, count, width), bf16),
        ((A, count, width), bf16),
        ((A - 1, count, width), bf16),
        ((A - 1, count, width), bf16),
    ]
    return pl.pallas_call(
        functools.partial(layer_kernel, n),
        out_shape=jax.ShapeDtypeStruct((count, width), bf16),
        in_specs=[vmem] * 4 + [smem] * 2 + [vmem] * 2 + [hbm] * 9,
        out_specs=vmem,
        scratch_shapes=[pltpu.VMEM(s, t) for s, t in scratch]
        + [
            pltpu.SemaphoreType.DMA((7,)),
            pltpu.SemaphoreType.DMA((count,)),
            pltpu.SemaphoreType.DMA((count,)),
            pltpu.SemaphoreType.DMA((9, n - 1)),
            pltpu.SemaphoreType.DMA((9, n - 1)),
        ],
        compiler_params=pltpu.CompilerParams(
            collective_id=0, has_side_effects=True, vmem_limit_bytes=62 * 1024 * 1024
        ),
        name="layer",
    )(
        tokens,
        norm_gain,
        head_gain.reshape(1, val),
        moe_gain,
        lambdas,
        lengths,
        routes.T,
        route_weights.T,
        query_weight.T,
        key_weight,
        value_weight,
        out_weight,
        cache_keys.reshape(count, ctx2, lanes),
        cache_values.reshape(count, ctx2, val),
        gate_weight,
        up_weight,
        down_weight,
    )


def solution(mesh):
    placed = (
        P(("grp", "ep"), None),
        P(),
        P(None, "ep"),
        P(),
        P(),
        P(None, "ep"),
        P(),
        P(),
        P(("grp", "ep"), None, None, None),
        P(("grp", "ep"), None, None, None),
        P(("grp", "ep")),
        P(),
        P("ep", None, None),
        P("ep", None, None),
        P("ep", None, None),
        P(("grp", "ep"), None),
        P(("grp", "ep"), None),
    )
    return jax.shard_map(
        functools.partial(local, mesh.shape["ep"]),
        mesh=mesh,
        in_specs=placed,
        out_specs=P(("grp", "ep"), None),
        check_vma=False,
    )
```
